32 devices in a mesh: ep: 8 (over z, core), tp: 4 (over y, x).
Axes of the slice: x: 2, y: 2, z: 4, core: 2. Of those that a mesh axis runs over, the one named last changes fastest.
Arguments:
- query_maps: bfloat16 [2048, 4096], P('ep', 'tp'), may hold values from -40 to 40
- key_maps: bfloat16 [2048, 4096], P('ep', 'tp'), may hold values from -40 to 40
- value_rows: bfloat16 [2048, 4096], P('ep', 'tp'), may hold values from -6 to 6
- head_lambda: float32 [16], P('tp'), may hold values from 0.3 to 0.8
- head_gain: float32 [256], replicated, may hold values from 0.1 to 1.9
- out_weight: bfloat16 [4096, 2048], P('tp'), may hold values from -0.125 to 0.125
- expert_rows: bfloat16 [1024, 2048], P('ep'), may hold values from -6 to 6
- expert_gain: float32 [2048], replicated, may hold values from 0.1 to 1.9
- routes: int32 [1024, 2], P('ep'), may hold values from 0 to 7, all different within a row; in each aligned block of 128 rows (0 to 127, 128 to 255, ...) at most 48 rows name the same one
- route_weights: float32 [1024, 2], P('ep'), may hold values from 0.2 to 1
- gate_weight: bfloat16 [8, 2048, 4096], P('ep', None, 'tp'), may hold values from -0.125 to 0.125
- up_weight: bfloat16 [8, 2048, 4096], P('ep', None, 'tp'), may hold values from -0.125 to 0.125
- down_weight: bfloat16 [8, 4096, 2048], P('ep', 'tp'), may hold values from -0.125 to 0.125
Outputs:
- mixed: bfloat16 [2048, 2048], P('ep', 'tp')
- expert_out: bfloat16 [1024, 2048], P('ep', 'tp')
The draws below stay inside these ranges and needn't reach their ends.
Inputs may be any that keep to these rules, and one draw needn't show every extreme that they name: `routes`: within the rows of one device (aligned blocks of 128 rows) no expert is named more than 48 times, and the 2 experts of a row differ.
All inputs are finite; a program needn't handle non-finite values.
Results may differ from the reference program's by a relative error of at most 0.018.
Values may be sent and summed in bfloat16 or wider, within the bound.
A program may use at most 128 MiB of HBM per device.

```python
import math
import jax
import jax.numpy as jnp
import numpy as np
from jax import lax

D = 2048
HEADS = 16
HEAD = 128
VHEAD = 256
FF = 4096
TOPK = 2
MOE_DEV = 128
TOKENS = 2048
MOE_TOK = 1024
EXPERTS = 8
CAP = 48
N_EP = 8
N_TP = 4


def draw_query_maps(key, part):
    base = jnp.clip(1.3 * jax.random.normal(jax.random.fold_in(key, 1), (TOKENS, HEADS * 2 * HEAD), jnp.float32), -7.8, 7.8)
    return base.astype(jnp.bfloat16)


def draw_key_maps(key, part):
    base = jnp.clip(1.3 * jax.random.normal(jax.random.fold_in(key, 2), (TOKENS, HEADS * 2 * HEAD), jnp.float32), -7.8, 7.8)
    base = base.reshape(TOKENS, HEADS, 2, HEAD)
    return base.reshape(TOKENS, HEADS * 2 * HEAD).astype(jnp.bfloat16)


def spiked(result, own_key, source, target, shards_of, factor):
    owner, partner = [(jnp.arange(result.shape[axis_at]) // (result.shape[axis_at] // shards_of)).reshape([-1 if axis == axis_at else 1 for axis in range(result.ndim)]) for axis_at in (source, target)]
    chosen = jax.random.permutation(own_key, shards_of)[partner]
    strong = (owner == chosen) | (owner == (partner + shards_of // 2) % shards_of)
    return jnp.where(strong, factor * result, result)


def level_of(stream_key, dims, cuts, low, top_value):
    loudness = 1.0
    for axis_at, blocks in cuts:
        steps = jax.random.uniform(jax.random.fold_in(jax.random.fold_in(stream_key, 6), axis_at), (blocks,), jnp.float32, low / len(cuts), top_value / len(cuts))
        loudness = loudness * jnp.repeat(jnp.exp(steps), dims[axis_at] // blocks).reshape((-1,) + (1,) * (len(dims) - 1 - axis_at))
    return loudness


def routed_block(stream_key, own, number, rows, amount, top, most, skew):
    order = jax.random.permutation(stream_key, amount)
    heavy_load, ordinary = load_shares(amount, rows * top, most, skew, True), load_shares(amount, rows * top, most, skew, False)
    places = jnp.arange(amount)

    def named(sizes, turn):
        used = int((sizes > 0).sum())
        fixed = max(1, used // 4)
        passed = fixed + (places - fixed + turn * (used - fixed)) % max(1, amount - fixed)
        return jnp.zeros((amount,), jnp.int32).at[order[jnp.where(places < fixed, places, passed)]].set(jnp.asarray(sizes, jnp.int32))

    sizes = jnp.where(number % 4 == 0, named(heavy_load, number // 4), named(ordinary, number - number // 4 - 1))
    mixed = jax.random.permutation(jax.random.fold_in(own, 3), amount)
    source_of, receiver = mixed[0:amount // 2 * 2:2], mixed[1:amount // 2 * 2:2]
    room = jnp.minimum(sizes[source_of] - 1, most - sizes[receiver]) // 2
    room = jnp.where((source_of == order[0]) | (receiver == order[0]) | (sizes[receiver] == 0), 0, jnp.maximum(room, 0))
    passed = jax.random.randint(jax.random.fold_in(own, 4), (amount // 2,), 0, 1 << 20) % (room + 1)
    sizes = sizes.at[source_of].add(-passed).at[receiver].add(passed)
    labels = jnp.searchsorted(jnp.cumsum(sizes), jnp.arange(rows * top), side="right").astype(jnp.int32)
    table = labels.reshape(top, rows).T
    table = table[jax.random.permutation(jax.random.fold_in(own, 1), rows)]
    turn = jax.random.randint(jax.random.fold_in(own, 2), (rows, 1), 0, top)
    return jnp.take_along_axis(table, (jnp.arange(top)[None, :] + turn) % top, axis=1)


def load_shares(number_of, total, bound, lean, full):
    portions = [(1 << 20) // math.isqrt(standing ** lean) + 1 for standing in range(1, number_of + 1)]
    largest = bound if full else min(bound, max(-(-total // number_of), total * portions[0] // sum(portions)))
    least = 1 if total - largest >= number_of - 1 else 0
    holding, surplus = [largest] + [least] * (number_of - 1), total - largest - least * (number_of - 1)
    while surplus > 0:
        free = [i for i in range(1, number_of) if holding[i] < largest] or [i for i in range(1, number_of) if holding[i] < bound]
        mass, budget = sum([portions[i] for i in free]), surplus
        for i in free:
            extra = min(bound - holding[i], max(1, budget * portions[i] // mass), surplus)
            holding[i] = holding[i] + extra
            surplus = surplus - extra
    return np.array(holding)


def centred(rng, extent, spread, bound, cuts=(), kind=jnp.bfloat16):
    array = spread * jax.random.normal(rng, extent, jnp.float32)
    if cuts:
        array = array * level_of(rng, extent, cuts, -0.22, 0.18)
    return jnp.clip(array, -bound, bound).astype(kind)


def heavy_noise(rng, extent, scale, most, split, heavy, kind=jnp.bfloat16):
    array = scale * jax.random.normal(rng, extent, jnp.float32)
    if split:
        array = array * level_of(rng, extent, split, -0.22, 0.18)
    return jnp.clip(spiked(array, jax.random.fold_in(rng, 3), *heavy), -most, most).astype(kind)


def setup_inputs(seed: int = 0) -> dict:
    key_list = jax.random.split(jax.random.key(seed), 14)
    query_maps = draw_query_maps(jax.random.fold_in(key_list[13], 71), 0)
    key_maps = draw_key_maps(jax.random.fold_in(key_list[13], 71), 0)
    value_rows = centred(key_list[2], (TOKENS, HEADS * VHEAD), 1.0, 6.0, ((0, 8), (1, 4)))
    head_lambda = jnp.clip(0.3 + 0.5 * jax.random.uniform(key_list[3], (HEADS,), jnp.float32) ** level_of(key_list[3], (HEADS,), ((0, 4),), -0.2, 0.2), 0.3, 0.8)
    head_gain = jnp.clip(1.0 + 0.18 * jax.random.normal(key_list[4], (VHEAD,), jnp.float32), 0.1, 1.9)
    out_weight = heavy_noise(key_list[5], (HEADS * VHEAD, D), (HEADS * VHEAD) ** -0.5, 0.125, ((0, 4),), (0, 1, 4, 2.0))
    expert_rows = centred(key_list[6], (MOE_TOK, D), 1.0, 6.0, ((0, 8),))
    expert_gain = jnp.clip(1.0 + 0.18 * jax.random.normal(key_list[7], (D,), jnp.float32), 0.1, 1.9)
    routes_keys = jax.random.split(jax.random.fold_in(key_list[8], 1), MOE_TOK // MOE_DEV)
    routes_turns = jax.random.permutation(jax.random.fold_in(key_list[8], 3), MOE_TOK // MOE_DEV)
    routes = jax.vmap(lambda own, number: routed_block(jax.random.fold_in(key_list[8], 2), own, number, MOE_DEV, EXPERTS, TOPK, CAP, 2))(routes_keys, routes_turns).reshape((MOE_TOK, TOPK))
    route_weights = jnp.clip(0.2 + 0.8 * jax.random.uniform(key_list[9], (MOE_TOK, TOPK), jnp.float32) ** level_of(key_list[9], (MOE_TOK, TOPK), ((0, 8),), -0.2, 0.2), 0.2, 1.0)
    gate_weight = centred(key_list[10], (EXPERTS, D, FF), D ** -0.5, 0.125, ((0, 8), (2, 4)))
    up_weight = centred(key_list[11], (EXPERTS, D, FF), D ** -0.5, 0.125, ((0, 8), (2, 4)))
    down_weight = heavy_noise(key_list[12], (EXPERTS, FF, D), FF ** -0.5, 0.125, ((0, 8), (1, 4)), (1, 2, 4, 2.0))
    return dict(query_maps=query_maps, key_maps=key_maps, value_rows=value_rows, head_lambda=head_lambda, head_gain=head_gain, out_weight=out_weight, expert_rows=expert_rows, expert_gain=expert_gain, routes=routes, route_weights=route_weights, gate_weight=gate_weight, up_weight=up_weight, down_weight=down_weight)


norm_eps = 1e-06
rope_base = 10000.0

def rope_turn(inputs, positions):
    half_dim = inputs.shape[-1] // 2
    inverse = rope_base ** (-2.0 * jnp.arange(half_dim, dtype=jnp.float32) / inputs.shape[-1])
    angles = positions.astype(jnp.float32)[:, None] * inverse[None, :]
    cos_table = jnp.cos(angles)[:, None, None, :]
    sin_table = jnp.sin(angles)[:, None, None, :]
    first_half = inputs[..., :half_dim]
    second_half = inputs[..., half_dim:]
    return jnp.concatenate([first_half * cos_table - second_half * sin_table, second_half * cos_table + first_half * sin_table], axis=-1)

def mixer_half(query_maps, key_maps, value_rows, head_lambda, head_gain, out_weight):
    positions = jnp.arange(TOKENS, dtype=jnp.int32)
    rotated_q = rope_turn(query_maps.astype(jnp.float32).reshape(TOKENS, HEADS, 2, HEAD), positions).astype(jnp.bfloat16)
    rotated_k = rope_turn(key_maps.astype(jnp.float32).reshape(TOKENS, HEADS, 2, HEAD), positions).astype(jnp.bfloat16)
    values_all = value_rows.reshape(TOKENS, HEADS, VHEAD)
    block_size = math.gcd(512, TOKENS)
    score_scale = HEAD ** (-0.5)

    def one_head(head_index):
        head_q = rotated_q[:, head_index].astype(jnp.float32)
        head_k = rotated_k[:, head_index].astype(jnp.float32)
        head_v = values_all[:, head_index].astype(jnp.float32)
        key_pos = jnp.arange(TOKENS, dtype=jnp.int32)

        def one_block(block_index):
            first_row = (block_index * block_size).astype(jnp.int32)
            block_q = lax.dynamic_slice_in_dim(head_q, first_row, block_size, 0)
            query_pos = first_row + jnp.arange(block_size, dtype=jnp.int32)
            scores = jnp.einsum('qmd,kmd->mqk', block_q, head_k) * score_scale
            causal = (key_pos[None, :] <= query_pos[:, None])[None]
            masked = jnp.where(causal, scores, -jnp.inf)
            peak = lax.optimization_barrier(jnp.max(masked, axis=-1, keepdims=True))
            expd = jnp.where(causal, jnp.exp(masked - peak), 0.0)
            probs = expd / lax.optimization_barrier(jnp.sum(expd, axis=-1, keepdims=True))
            rounded = lax.optimization_barrier(probs.astype(jnp.bfloat16))
            map_out = jnp.einsum('mqk,ke->mqe', rounded.astype(jnp.float32), head_v)
            difference = map_out[0] - head_lambda[head_index] * map_out[1]
            normed = difference * lax.rsqrt(lax.optimization_barrier(jnp.mean(difference * difference, axis=-1, keepdims=True)) + norm_eps) * head_gain
            return normed.astype(jnp.bfloat16)
        blocks = lax.map(one_block, jnp.arange(TOKENS // block_size, dtype=jnp.int32))
        return blocks.reshape(TOKENS, VHEAD)
    per_head = lax.map(one_head, jnp.arange(HEADS, dtype=jnp.int32))
    group_size = HEADS // N_TP
    grouped = per_head.reshape(N_TP, group_size, TOKENS, VHEAD)
    weight_groups = out_weight.reshape(N_TP, group_size, VHEAD, D)

    def add_group(running, pieces):
        group_heads, group_weight = pieces
        partial_value = jnp.einsum('hte,hed->td', group_heads.astype(jnp.float32), group_weight.astype(jnp.float32))
        rounded = lax.optimization_barrier(partial_value.astype(jnp.bfloat16))
        return (running + rounded.astype(jnp.float32), None)
    summed, _ = lax.scan(add_group, jnp.zeros((TOKENS, D), jnp.float32), (grouped, weight_groups))
    return summed.astype(jnp.bfloat16)

def expert_half(expert_rows, expert_gain, routes, route_weights, gate_weight, up_weight, down_weight):
    inputs = expert_rows.astype(jnp.float32)
    normed = (inputs * lax.rsqrt(lax.optimization_barrier(jnp.mean(inputs * inputs, axis=-1, keepdims=True)) + norm_eps) * expert_gain).astype(jnp.bfloat16)
    expert_ids = routes.reshape(N_EP, MOE_DEV * TOPK)
    one_hot = (expert_ids[..., None] == jnp.arange(EXPERTS, dtype=jnp.int32)).astype(jnp.int32)
    slot_index = lax.optimization_barrier(jnp.sum((jnp.cumsum(one_hot, axis=1) - one_hot) * one_hot, axis=-1)).astype(jnp.int32)
    source_block = jnp.zeros_like(expert_ids) + jnp.arange(N_EP, dtype=jnp.int32)[:, None]
    repeated = jnp.repeat(normed.reshape(N_EP, MOE_DEV, D), TOPK, axis=1)
    buffer = jnp.zeros((EXPERTS, N_EP, CAP, D), normed.dtype).at[expert_ids, source_block, slot_index].set(repeated)
    group_width = FF // N_TP

    def run_one(pieces):
        slots, gate_one, up_one, down_one = pieces
        flat_rows = slots.reshape(N_EP * CAP, D)
        gate_values = jnp.dot(flat_rows, gate_one, preferred_element_type=jnp.float32)
        up_values = jnp.dot(flat_rows, up_one, preferred_element_type=jnp.float32)
        hidden = (jax.nn.silu(gate_values) * up_values).astype(jnp.bfloat16)
        hidden_groups = jnp.transpose(hidden.reshape(N_EP * CAP, N_TP, group_width), (1, 0, 2))
        down_groups = down_one.reshape(N_TP, group_width, D)

        def add_group(running, pieces_inner):
            hidden_part, down_part = pieces_inner
            partial_value = jnp.dot(hidden_part, down_part, preferred_element_type=jnp.float32)
            rounded = lax.optimization_barrier(partial_value.astype(jnp.bfloat16))
            return (running + rounded.astype(jnp.float32), None)
        summed, _ = lax.scan(add_group, jnp.zeros((N_EP * CAP, D), jnp.float32), (hidden_groups, down_groups))
        return summed.astype(jnp.bfloat16).reshape(N_EP, CAP, D)
    results = lax.map(run_one, (buffer, gate_weight, up_weight, down_weight))
    picked = results[expert_ids, source_block, slot_index].reshape(MOE_TOK, TOPK, D)
    combined = lax.optimization_barrier(jnp.sum(route_weights[..., None] * picked.astype(jnp.float32), axis=1))
    return combined.astype(jnp.bfloat16)

def reference(query_maps, key_maps, value_rows, head_lambda, head_gain, out_weight, expert_rows, expert_gain, routes, route_weights, gate_weight, up_weight, down_weight):
    mixed = mixer_half(query_maps, key_maps, value_rows, head_lambda, head_gain, out_weight)
    expert_out = expert_half(expert_rows, expert_gain, routes, route_weights, gate_weight, up_weight, down_weight)
    return (mixed, expert_out)
```

```python
import functools

import jax
import jax.numpy as jnp
from jax import lax
from jax.experimental import pallas as pl
from jax.experimental.pallas import tpu as pltpu
from jax.sharding import PartitionSpec as P

norm_eps = 1e-06
rope_base = 10000.0


def rope_turn(inputs, positions):
    half_dim = inputs.shape[-1] // 2
    inverse = rope_base ** (-2.0 * jnp.arange(half_dim, dtype=jnp.float32) / inputs.shape[-1])
    angles = positions.astype(jnp.float32)[:, None] * inverse[None, :]
    cos_table = jnp.cos(angles)[:, None, None, :]
    sin_table = jnp.sin(angles)[:, None, None, :]
    first_half = inputs[..., :half_dim]
    second_half = inputs[..., half_dim:]
    return jnp.concatenate(
        [
            first_half * cos_table - second_half * sin_table,
            second_half * cos_table + first_half * sin_table,
        ],
        axis=-1,
    )


def mixer_half(query_maps, key_maps, value_rows, head_lambda, head_gain, out_weight):
    row_count = query_maps.shape[0]
    head_count = head_lambda.shape[0]
    head_dim = query_maps.shape[1] // (2 * head_count)
    value_dim = value_rows.shape[1] // head_count
    model_width = out_weight.shape[1]
    score_scale = head_dim ** (-0.5)
    offset = lax.axis_index("ep") * row_count
    positions = offset + jnp.arange(row_count, dtype=jnp.int32)
    last_row = offset + row_count - 1
    rotated_q = rope_turn(
        query_maps.astype(jnp.float32).reshape(row_count, head_count, 2, head_dim), positions
    ).astype(jnp.bfloat16)
    rotated_k = rope_turn(
        key_maps.astype(jnp.float32).reshape(row_count, head_count, 2, head_dim), positions
    ).astype(jnp.bfloat16)
    rotated_k = rotated_k.reshape(row_count, head_count * 2 * head_dim)
    initial = (
        jnp.full((head_count, 2, row_count), -1e30, jnp.float32),
        jnp.zeros((head_count, 2, row_count), jnp.float32),
        jnp.zeros((head_count, 2, row_count, value_dim), jnp.float32),
    )
    piece_k = lax.all_gather(rotated_k, "ep", axis=0, tiled=True)
    piece_v = lax.all_gather(value_rows, "ep", axis=0, tiled=True)
    piece_len = piece_k.shape[0]
    block_size = 1024

    def attend(state):

        def fold_step(inner, block_index):
            block_start = block_index * block_size
            block_k = lax.dynamic_slice_in_dim(piece_k, block_start, block_size, 0).reshape(
                block_size, head_count, 2, head_dim
            )
            block_v = lax.dynamic_slice_in_dim(piece_v, block_start, block_size, 0).reshape(
                block_size, head_count, value_dim
            )
            scores = (
                jnp.einsum(
                    "qhmd,khmd->hmqk", rotated_q, block_k, preferred_element_type=jnp.float32
                )
                * score_scale
            )
            key_pos = block_start + jnp.arange(block_size, dtype=jnp.int32)
            causal = key_pos[None, :] <= positions[:, None]
            masked = jnp.where(causal, scores, -1e30)
            run_max, run_sum, run_acc = inner
            new_max = jnp.maximum(run_max, jnp.max(masked, axis=-1))
            expd = jnp.where(causal, jnp.exp(masked - new_max[..., None]), 0.0)
            rescale = jnp.exp(run_max - new_max)
            new_sum = run_sum * rescale + jnp.sum(expd, axis=-1)
            new_acc = run_acc * rescale[..., None] + jnp.einsum(
                "hmqk,khe->hmqe",
                expd.astype(jnp.bfloat16),
                block_v,
                preferred_element_type=jnp.float32,
            )
            return ((new_max, new_sum, new_acc), None)

        result, _ = lax.scan(fold_step, state, jnp.arange(piece_len // block_size, dtype=jnp.int32))
        return result

    def skip_piece(state):
        return state

    run_max, run_sum, run_acc = lax.cond(jnp.int32(0) <= last_row, attend, skip_piece, initial)
    first_map = run_acc[:, 0] / run_sum[:, 0][..., None]
    second_map = run_acc[:, 1] / run_sum[:, 1][..., None]
    difference = first_map - head_lambda[:, None, None] * second_map
    head_out = (
        difference
        * lax.rsqrt(jnp.mean(difference * difference, axis=-1, keepdims=True) + norm_eps)
        * head_gain
    ).astype(jnp.bfloat16)
    partial_value = jnp.einsum(
        "hqe,hed->qd",
        head_out,
        out_weight.reshape(head_count, value_dim, model_width),
        preferred_element_type=jnp.float32,
    )
    return lax.psum_scatter(
        partial_value.astype(jnp.bfloat16), "tp", scatter_dimension=1, tiled=True
    )


def expert_half(
    expert_rows, expert_gain, routes, route_weights, gate_weight, up_weight, down_weight
):
    ep_count = lax.axis_size("ep")
    tp_count = lax.axis_size("tp")
    row_count, model_width = expert_rows.shape
    pick_count = routes.shape[1]
    capacity = 3 * row_count * pick_count // (2 * ep_count)
    column_count = model_width // tp_count
    inputs = expert_rows.astype(jnp.float32)
    normed = (
        inputs
        * lax.rsqrt(jnp.mean(inputs * inputs, axis=-1, keepdims=True) + norm_eps)
        * expert_gain
    ).astype(jnp.bfloat16)
    expert_ids = routes.reshape(-1)
    one_hot = (expert_ids[:, None] == jnp.arange(ep_count, dtype=jnp.int32)[None, :]).astype(
        jnp.int32
    )
    slot_index = jnp.sum((jnp.cumsum(one_hot, axis=0) - one_hot) * one_hot, axis=1)
    source_row = jnp.arange(row_count * pick_count, dtype=jnp.int32) // pick_count
    empty = jnp.zeros((ep_count, capacity, normed.shape[1]), jnp.bfloat16)
    arrived = lax.all_to_all(
        empty.at[expert_ids, slot_index].set(normed[source_row]),
        "ep",
        split_axis=0,
        concat_axis=0,
        tiled=True,
    )
    slot_count = arrived.shape[1]
    flat_rows = arrived.reshape(ep_count * slot_count, model_width)
    gate_values = jnp.dot(flat_rows, gate_weight[0], preferred_element_type=jnp.float32)
    up_values = jnp.dot(flat_rows, up_weight[0], preferred_element_type=jnp.float32)
    hidden = (jax.nn.silu(gate_values) * up_values).astype(jnp.bfloat16)
    partial_value = jnp.dot(hidden, down_weight[0], preferred_element_type=jnp.float32).reshape(
        ep_count, slot_count, model_width
    )
    summed = lax.psum_scatter(
        partial_value.astype(jnp.bfloat16), "tp", scatter_dimension=2, tiled=True
    )
    returned = lax.all_to_all(summed, "ep", split_axis=0, concat_axis=0, tiled=True)
    picked = returned[expert_ids, slot_index].reshape(row_count, pick_count, column_count)
    combined = jnp.sum(route_weights[..., None] * picked.astype(jnp.float32), axis=1)
    return combined.astype(jnp.bfloat16)


MESH = pl.DeviceIdType.MESH


def remote(source, target, send_sem, recv_sem, device):
    return pltpu.make_async_remote_copy(
        src_ref=source,
        dst_ref=target,
        send_sem=send_sem,
        recv_sem=recv_sem,
        device_id=device,
        device_id_type=MESH,
    )


def greet(devices):
    barrier = pltpu.get_barrier_semaphore()
    for device in devices:
        pl.semaphore_signal(barrier, inc=1, device_id=device, device_id_type=MESH)
    pl.semaphore_wait(barrier, len(devices))


def front_kernel(
    n_ep,
    n_tp,
    slots_ref,
    select_ref,
    route_weights_ref,
    query_ref,
    key_ref,
    value_ref,
    cos_ref,
    sin_ref,
    gate_hbm,
    up_hbm,
    down_hbm,
    expert_ref,
    all_ref,
    packed,
    gathered,
    gate_vmem,
    up_vmem,
    down_vmem,
    hidden,
    partial,
    arrived,
    summed,
    returned,
    weight_sem,
    local_sem,
    disp_send,
    disp_recv,
    gath_send,
    gath_recv,
    part_send,
    part_recv,
    ret_send,
    ret_recv,
    qkv_send,
    qkv_recv,
    pair_send,
    pair_recv,
):
    ep = lax.axis_index("ep")
    tp = lax.axis_index("tp")
    n_z = n_ep // 2
    z, core = ep // 2, lax.rem(ep, 2)
    capacity, width = slots_ref.shape[1:]
    rows = n_ep * capacity
    head_width = packed.shape[2] // 3
    half = head_width // 2
    weights = [
        pltpu.make_async_copy(gate_hbm, gate_vmem, weight_sem.at[0]),
        pltpu.make_async_copy(up_hbm, up_vmem, weight_sem.at[1]),
        pltpu.make_async_copy(down_hbm, down_vmem, weight_sem.at[2]),
    ]
    for copy in weights:
        copy.start()
    greet(
        [{"ep": lax.rem(ep + d, n_ep)} for d in range(1, n_ep)]
        + [{"tp": lax.rem(tp + d, n_tp)} for d in range(1, n_tp)]
    )
    mine = tp * n_ep + ep
    dispatch = [pltpu.make_async_copy(slots_ref.at[ep], gathered.at[mine], local_sem.at[0])]
    for d in range(1, n_ep):
        target = lax.rem(ep + d, n_ep)
        dispatch.append(
            remote(
                slots_ref.at[target],
                gathered.at[mine],
                disp_send.at[d],
                disp_recv.at[d],
                {"ep": target},
            )
        )
    for copy in dispatch:
        copy.start()

    for head in range(n_z):
        for index, ref in ((0, query_ref), (1, key_ref)):
            for m in range(2):
                at = head * head_width + m * half
                entry = ref[:, at : at + half].astype(jnp.float32)
                turned = entry * cos_ref[...] + pltpu.roll(entry, half // 2, 1) * sin_ref[...]
                to = index * head_width + m * half
                packed[head, :, to : to + half] = turned.astype(jnp.bfloat16)
        packed[head, :, 2 * head_width :] = value_ref[
            :, head * head_width : (head + 1) * head_width
        ]
    exchange = [pltpu.make_async_copy(packed.at[z], all_ref.at[ep], local_sem.at[1])]
    for d in range(1, n_z):
        target = lax.rem(z + d, n_z)
        exchange.append(
            remote(
                packed.at[target],
                all_ref.at[ep],
                qkv_send.at[d],
                qkv_recv.at[d],
                {"ep": 2 * target + core},
            )
        )
    for copy in exchange:
        copy.start()

    spread = []
    for d in range(n_ep):
        source = lax.rem(ep + n_ep - d, n_ep)
        if d == 0:
            dispatch[0].wait()
        else:
            dispatch[d].wait_recv()
        slot = gathered.at[tp * n_ep + source]
        for t in range(1, n_tp):
            copy = remote(
                slot,
                slot,
                gath_send.at[d * n_tp + t],
                gath_recv.at[d * n_tp + t],
                {"tp": lax.rem(tp + t, n_tp)},
            )
            copy.start()
            spread.append(copy)
    for copy in spread:
        copy.wait_recv()
    weights[0].wait()
    weights[1].wait()
    tile = 256

    def hidden_tile(j, carry):
        columns = pl.ds(pl.multiple_of(j * tile, tile), tile)
        gate = jnp.zeros((rows, tile), jnp.float32)
        up = jnp.zeros((rows, tile), jnp.float32)
        for i in range(n_tp):
            block = gathered[i * n_ep : (i + 1) * n_ep].reshape(rows, width)
            gate += jnp.dot(
                block,
                gate_vmem[0, i * width : (i + 1) * width, columns],
                preferred_element_type=jnp.float32,
            )
            up += jnp.dot(
                block,
                up_vmem[0, i * width : (i + 1) * width, columns],
                preferred_element_type=jnp.float32,
            )
        hidden[:, columns] = (gate / (1.0 + jnp.exp(-gate)) * up).astype(jnp.bfloat16)
        return carry

    lax.fori_loop(0, hidden.shape[1] // tile, hidden_tile, 0)
    weights[2].wait()
    scatter = []
    for d in list(range(1, n_tp)) + [0]:
        target = lax.rem(tp + d, n_tp)
        columns = pl.ds(pl.multiple_of(target * width, width), width)
        partial[d] = jnp.dot(
            hidden[...], down_vmem[0, :, columns], preferred_element_type=jnp.float32
        ).astype(jnp.bfloat16)
        if d:
            copy = remote(
                partial.at[d], arrived.at[d], part_send.at[d], part_recv.at[d], {"tp": target}
            )
            copy.start()
            scatter.append(copy)
    total = partial[0].astype(jnp.float32)
    for d in range(1, n_tp):
        scatter[d - 1].wait_recv()
        total += arrived[d].astype(jnp.float32)
    summed[...] = total.astype(jnp.bfloat16).reshape(n_ep, capacity, width)
    back = [pltpu.make_async_copy(summed.at[ep], returned.at[ep], local_sem.at[2])]
    for d in range(1, n_ep):
        target = lax.rem(ep + d, n_ep)
        back.append(
            remote(
                summed.at[target],
                returned.at[ep],
                ret_send.at[d],
                ret_recv.at[d],
                {"ep": target},
            )
        )
    for copy in back:
        copy.start()

    pairs = []
    for d in range(n_z):
        source = 2 * lax.rem(z + n_z - d, n_z) + core
        if d == 0:
            exchange[0].wait()
        else:
            exchange[d].wait_recv()
        part = all_ref.at[source, :, pl.ds(head_width, 2 * head_width)]
        copy = remote(part, part, pair_send.at[d], pair_recv.at[d], {"ep": ep + 1 - 2 * core})
        copy.start()
        pairs.append(copy)

    back[0].wait()
    for copy in back[1:]:
        copy.wait_recv()
    flat = returned[...].reshape(rows, width)
    result = jnp.zeros(expert_ref.shape, jnp.float32)
    for k in range(select_ref.shape[0]):
        picked = jnp.dot(select_ref[k], flat, preferred_element_type=jnp.float32)
        result += route_weights_ref[:, k : k + 1] * picked
    expert_ref[...] = result.astype(expert_ref.dtype)
    for copy in pairs:
        copy.wait_recv()
    for copy in dispatch[1:] + exchange[1:] + spread + scatter + back[1:] + pairs:
        copy.wait_send()


def back_kernel(
    n_ep,
    n_tp,
    all_ref,
    lambda_ref,
    gain_ref,
    weight_hbm,
    mixed_ref,
    weight_vmem,
    heads,
    landed,
    partial,
    arrived,
    weight_sem,
    head_send,
    head_recv,
    part_send,
    part_recv,
):
    ep = lax.axis_index("ep")
    tp = lax.axis_index("tp")
    n_z = n_ep // 2
    z, core = ep // 2, lax.rem(ep, 2)
    row_count = all_ref.shape[1]
    value_width = gain_ref.shape[1]
    half = value_width // 2
    width = mixed_ref.shape[1]
    weight = pltpu.make_async_copy(weight_hbm, weight_vmem, weight_sem)
    weight.start()
    greet(
        [{"ep": 2 * lax.rem(z + d, n_z) + core} for d in range(1, n_z)]
        + [{"tp": lax.rem(tp + d, n_tp)} for d in range(1, n_tp)]
    )
    scale = half ** (-0.5)
    pair_rows = 2 * row_count
    row = lax.broadcasted_iota(jnp.int32, (row_count, pair_rows), 0) + core * row_count
    causal = lax.broadcasted_iota(jnp.int32, (row_count, pair_rows), 1) <= row

    def sender(block):
        return remote(
            heads.at[block],
            landed.at[z],
            head_send.at[block],
            head_recv.at[z],
            {"ep": 2 * block + core},
        )

    def keeper(block):
        return pltpu.make_async_copy(heads.at[block], landed.at[block], head_recv.at[block])

    for block in range(n_z - 1, -1, -1):
        maps = []
        for m in range(2):
            query = all_ref[2 * block + core, :, m * half : (m + 1) * half]
            pieces = []
            for pair in range(block + 1):
                at = value_width + m * half
                keys = all_ref[2 * pair : 2 * pair + 2, :, at : at + half].reshape(pair_rows, half)
                scores = lax.dot_general(
                    query, keys, (((1,), (1,)), ((), ())), preferred_element_type=jnp.float32
                )
                scores = scores * scale
                if pair == block:
                    scores = jnp.where(causal, scores, -1e30)
                pieces.append(scores)
            peak = functools.reduce(
                jnp.maximum, [jnp.max(piece, axis=1, keepdims=True) for piece in pieces]
            )
            total = jnp.zeros((row_count, 1), jnp.float32)
            outcome = jnp.zeros((row_count, value_width), jnp.float32)
            for pair in range(block + 1):
                expd = jnp.exp(pieces[pair] - peak)
                total += jnp.sum(expd, axis=1, keepdims=True)
                values = all_ref[2 * pair : 2 * pair + 2, :, 2 * value_width :].reshape(
                    pair_rows, value_width
                )
                outcome += jnp.dot(
                    expd.astype(jnp.bfloat16), values, preferred_element_type=jnp.float32
                )
            maps.append(outcome / total)
        difference = maps[0] - lambda_ref[...] * maps[1]
        mean = jnp.mean(difference * difference, axis=1, keepdims=True)
        heads[block] = (difference * lax.rsqrt(mean + norm_eps) * gain_ref[...]).astype(
            jnp.bfloat16
        )

        @pl.when(z == block)
        def _():
            keeper(block).start()

        @pl.when(z != block)
        def _():
            sender(block).start()

    for block in range(n_z):
        keeper(block).wait()
    weight.wait()
    scatter = []
    for d in list(range(1, n_tp)) + [0]:
        target = lax.rem(tp + d, n_tp)
        columns = pl.ds(pl.multiple_of(target * width, width), width)
        product = jnp.zeros((row_count, width), jnp.float32)
        for h in range(n_z):
            product += jnp.dot(
                landed[h],
                weight_vmem[h * value_width : (h + 1) * value_width, columns],
                preferred_element_type=jnp.float32,
            )
        partial[d] = product.astype(jnp.bfloat16)
        if d:
            copy = remote(
                partial.at[d], arrived.at[d], part_send.at[d], part_recv.at[d], {"tp": target}
            )
            copy.start()
            scatter.append(copy)
    total = partial[0].astype(jnp.float32)
    for d in range(1, n_tp):
        scatter[d - 1].wait_recv()
        total += arrived[d].astype(jnp.float32)
    mixed_ref[...] = total.astype(jnp.bfloat16)
    for copy in scatter:
        copy.wait_send()
    for block in range(n_z):

        @pl.when(z != block)
        def _():
            sender(block).wait_send()


def fused(
    query_maps,
    key_maps,
    value_rows,
    head_lambda,
    head_gain,
    out_weight,
    expert_rows,
    expert_gain,
    routes,
    route_weights,
    gate_weight,
    up_weight,
    down_weight,
):
    n_ep = lax.axis_size("ep")
    n_tp = lax.axis_size("tp")
    n_z = n_ep // 2
    ep = lax.axis_index("ep")
    tp = lax.axis_index("tp")
    row_count = query_maps.shape[0]
    head_width = query_maps.shape[1] // n_z
    head_dim = head_width // 2
    token_count, model_width = expert_rows.shape
    pick_count = routes.shape[1]
    capacity = 3 * token_count * pick_count // (2 * n_ep)
    width = model_width // n_tp
    hidden_width = gate_weight.shape[2]
    slot_rows = n_ep * capacity

    positions = ep * row_count + jnp.arange(row_count, dtype=jnp.int32)
    half_dim = head_dim // 2
    inverse = rope_base ** (-2.0 * jnp.arange(half_dim, dtype=jnp.float32) / head_dim)
    angles = positions.astype(jnp.float32)[:, None] * inverse[None, :]
    cosine, sine = jnp.cos(angles), jnp.sin(angles)
    cos_table = jnp.concatenate([cosine, cosine], axis=1)
    sin_table = jnp.concatenate([-sine, sine], axis=1)

    inputs = expert_rows.astype(jnp.float32)
    inverse_norm = lax.rsqrt(jnp.mean(inputs * inputs, axis=-1, keepdims=True) + norm_eps)
    part_rows = lax.dynamic_slice_in_dim(expert_rows, tp * width, width, 1).astype(jnp.float32)
    part_gain = lax.dynamic_slice_in_dim(expert_gain, tp * width, width, 0)
    normed = (part_rows * inverse_norm * part_gain).astype(jnp.bfloat16)
    picks = jnp.arange(token_count * pick_count, dtype=jnp.int32)
    expert_ids = routes.reshape(-1)
    earlier = (expert_ids[:, None] == expert_ids[None, :]) & (picks[None, :] < picks[:, None])
    slot_index = jnp.sum(earlier.astype(jnp.int32), axis=1)
    place = (expert_ids * capacity + slot_index).reshape(token_count, pick_count).T
    select = place[:, :, None] == jnp.arange(slot_rows, dtype=jnp.int32)[None, None, :]
    chosen = jnp.any(select, axis=0).astype(jnp.bfloat16)
    slots = lax.dot_general(
        chosen, normed, (((0,), (0,)), ((), ())), preferred_element_type=jnp.float32
    ).astype(jnp.bfloat16)
    slots = slots.reshape(n_ep, capacity, width)

    vmem = pl.BlockSpec(memory_space=pltpu.VMEM)
    hbm = pl.BlockSpec(memory_space=pl.ANY)
    dma = pltpu.SemaphoreType.DMA
    bf16 = jnp.bfloat16
    expert_out, everything = pl.pallas_call(
        functools.partial(front_kernel, n_ep, n_tp),
        out_shape=(
            jax.ShapeDtypeStruct((token_count, width), bf16),
            jax.ShapeDtypeStruct((n_ep, row_count, 3 * head_width), bf16),
        ),
        in_specs=[vmem] * 8 + [hbm] * 3,
        out_specs=(vmem, vmem),
        scratch_shapes=[
            pltpu.VMEM((n_z, row_count, 3 * head_width), bf16),
            pltpu.VMEM((n_tp * n_ep, capacity, width), bf16),
            pltpu.VMEM(gate_weight.shape, bf16),
            pltpu.VMEM(up_weight.shape, bf16),
            pltpu.VMEM(down_weight.shape, bf16),
            pltpu.VMEM((slot_rows, hidden_width), bf16),
            pltpu.VMEM((n_tp, slot_rows, width), bf16),
            pltpu.VMEM((n_tp, slot_rows, width), bf16),
            pltpu.VMEM((n_ep, capacity, width), bf16),
            pltpu.VMEM((n_ep, capacity, width), bf16),
            dma((3,)),
            dma((3,)),
            dma((n_ep,)),
            dma((n_ep,)),
            dma((n_ep * n_tp,)),
            dma((n_ep * n_tp,)),
            dma((n_tp,)),
            dma((n_tp,)),
            dma((n_ep,)),
            dma((n_ep,)),
            dma((n_z,)),
            dma((n_z,)),
            dma((n_z,)),
            dma((n_z,)),
        ],
        compiler_params=pltpu.CompilerParams(
            collective_id=0, has_side_effects=True, vmem_limit_bytes=56 * 1024 * 1024
        ),
        name="front",
    )(
        slots,
        select.astype(bf16),
        route_weights,
        query_maps,
        key_maps,
        value_rows,
        cos_table,
        sin_table,
        gate_weight,
        up_weight,
        down_weight,
    )
    mixed = pl.pallas_call(
        functools.partial(back_kernel, n_ep, n_tp),
        out_shape=jax.ShapeDtypeStruct((row_count, width), bf16),
        in_specs=[vmem] * 3 + [hbm],
        out_specs=vmem,
        scratch_shapes=[
            pltpu.VMEM(out_weight.shape, bf16),
            pltpu.VMEM((n_z, row_count, head_width), bf16),
            pltpu.VMEM((n_z, row_count, head_width), bf16),
            pltpu.VMEM((n_tp, row_count, width), bf16),
            pltpu.VMEM((n_tp, row_count, width), bf16),
            dma,
            dma((n_z,)),
            dma((n_z,)),
            dma((n_tp,)),
            dma((n_tp,)),
        ],
        compiler_params=pltpu.CompilerParams(
            collective_id=1, has_side_effects=True, vmem_limit_bytes=56 * 1024 * 1024
        ),
        name="back",
    )(
        everything,
        lax.dynamic_slice_in_dim(head_lambda, ep // 2, 1, 0).reshape(1, 1),
        head_gain.reshape(1, head_width),
        out_weight,
    )
    return (mixed, expert_out)


def on_device(
    query_maps,
    key_maps,
    value_rows,
    head_lambda,
    head_gain,
    out_weight,
    expert_rows,
    expert_gain,
    routes,
    route_weights,
    gate_weight,
    up_weight,
    down_weight,
):
    n_ep = lax.axis_size("ep")
    head_count = head_lambda.shape[0]
    capacity = 3 * expert_rows.shape[0] * routes.shape[1] // (2 * n_ep)
    if (
        2 * head_count == n_ep
        and capacity % 16 == 0
        and value_rows.shape[1] == query_maps.shape[1] == 256 * head_count
    ):
        return fused(
            query_maps,
            key_maps,
            value_rows,
            head_lambda,
            head_gain,
            out_weight,
            expert_rows,
            expert_gain,
            routes,
            route_weights,
            gate_weight,
            up_weight,
            down_weight,
        )
    mixed = mixer_half(query_maps, key_maps, value_rows, head_lambda, head_gain, out_weight)
    expert_out = expert_half(
        expert_rows, expert_gain, routes, route_weights, gate_weight, up_weight, down_weight
    )
    return (mixed, expert_out)


def solution(mesh):
    placed = (
        P("ep", "tp"),
        P("ep", "tp"),
        P("ep", "tp"),
        P("tp"),
        P(),
        P("tp", None),
        P("ep", None),
        P(),
        P("ep", None),
        P("ep", None),
        P("ep", None, "tp"),
        P("ep", None, "tp"),
        P("ep", "tp", None),
    )
    return jax.shard_map(
        on_device,
        mesh=mesh,
        in_specs=placed,
        out_specs=(P("ep", "tp"), P("ep", "tp")),
        check_vma=False,
    )
```

```python
import functools

import jax
import jax.numpy as jnp
from jax import lax
from jax.experimental import pallas as pl
from jax.experimental.pallas import tpu as pltpu
from jax.sharding import PartitionSpec as P

norm_eps = 1e-06
rope_base = 10000.0


def rope_turn(inputs, positions):
    half_dim = inputs.shape[-1] // 2
    inverse = rope_base ** (-2.0 * jnp.arange(half_dim, dtype=jnp.float32) / inputs.shape[-1])
    angles = positions.astype(jnp.float32)[:, None] * inverse[None, :]
    cos_table = jnp.cos(angles)[:, None, None, :]
    sin_table = jnp.sin(angles)[:, None, None, :]
    first_half = inputs[..., :half_dim]
    second_half = inputs[..., half_dim:]
    return jnp.concatenate(
        [
            first_half * cos_table - second_half * sin_table,
            second_half * cos_table + first_half * sin_table,
        ],
        axis=-1,
    )


def mixer_half(query_maps, key_maps, value_rows, head_lambda, head_gain, out_weight):
    row_count = query_maps.shape[0]
    head_count = head_lambda.shape[0]
    head_dim = query_maps.shape[1] // (2 * head_count)
    value_dim = value_rows.shape[1] // head_count
    model_width = out_weight.shape[1]
    score_scale = head_dim ** (-0.5)
    offset = lax.axis_index("ep") * row_count
    positions = offset + jnp.arange(row_count, dtype=jnp.int32)
    last_row = offset + row_count - 1
    rotated_q = rope_turn(
        query_maps.astype(jnp.float32).reshape(row_count, head_count, 2, head_dim), positions
    ).astype(jnp.bfloat16)
    rotated_k = rope_turn(
        key_maps.astype(jnp.float32).reshape(row_count, head_count, 2, head_dim), positions
    ).astype(jnp.bfloat16)
    rotated_k = rotated_k.reshape(row_count, head_count * 2 * head_dim)
    initial = (
        jnp.full((head_count, 2, row_count), -1e30, jnp.float32),
        jnp.zeros((head_count, 2, row_count), jnp.float32),
        jnp.zeros((head_count, 2, row_count, value_dim), jnp.float32),
    )
    piece_k = lax.all_gather(rotated_k, "ep", axis=0, tiled=True)
    piece_v = lax.all_gather(value_rows, "ep", axis=0, tiled=True)
    piece_len = piece_k.shape[0]
    block_size = 1024

    def attend(state):

        def fold_step(inner, block_index):
            block_start = block_index * block_size
            block_k = lax.dynamic_slice_in_dim(piece_k, block_start, block_size, 0).reshape(
                block_size, head_count, 2, head_dim
            )
            block_v = lax.dynamic_slice_in_dim(piece_v, block_start, block_size, 0).reshape(
                block_size, head_count, value_dim
            )
            scores = (
                jnp.einsum(
                    "qhmd,khmd->hmqk", rotated_q, block_k, preferred_element_type=jnp.float32
                )
                * score_scale
            )
            key_pos = block_start + jnp.arange(block_size, dtype=jnp.int32)
            causal = key_pos[None, :] <= positions[:, None]
            masked = jnp.where(causal, scores, -1e30)
            run_max, run_sum, run_acc = inner
            new_max = jnp.maximum(run_max, jnp.max(masked, axis=-1))
            expd = jnp.where(causal, jnp.exp(masked - new_max[..., None]), 0.0)
            rescale = jnp.exp(run_max - new_max)
            new_sum = run_sum * rescale + jnp.sum(expd, axis=-1)
            new_acc = run_acc * rescale[..., None] + jnp.einsum(
                "hmqk,khe->hmqe",
                expd.astype(jnp.bfloat16),
                block_v,
                preferred_element_type=jnp.float32,
            )
            return ((new_max, new_sum, new_acc), None)

        result, _ = lax.scan(fold_step, state, jnp.arange(piece_len // block_size, dtype=jnp.int32))
        return result

    def skip_piece(state):
        return state

    run_max, run_sum, run_acc = lax.cond(jnp.int32(0) <= last_row, attend, skip_piece, initial)
    first_map = run_acc[:, 0] / run_sum[:, 0][..., None]
    second_map = run_acc[:, 1] / run_sum[:, 1][..., None]
    difference = first_map - head_lambda[:, None, None] * second_map
    head_out = (
        difference
        * lax.rsqrt(jnp.mean(difference * difference, axis=-1, keepdims=True) + norm_eps)
        * head_gain
    ).astype(jnp.bfloat16)
    partial_value = jnp.einsum(
        "hqe,hed->qd",
        head_out,
        out_weight.reshape(head_count, value_dim, model_width),
        preferred_element_type=jnp.float32,
    )
    return lax.psum_scatter(
        partial_value.astype(jnp.bfloat16), "tp", scatter_dimension=1, tiled=True
    )


def expert_half(
    expert_rows, expert_gain, routes, route_weights, gate_weight, up_weight, down_weight
):
    ep_count = lax.axis_size("ep")
    tp_count = lax.axis_size("tp")
    row_count, model_width = expert_rows.shape
    pick_count = routes.shape[1]
    capacity = 3 * row_count * pick_count // (2 * ep_count)
    column_count = model_width // tp_count
    inputs = expert_rows.astype(jnp.float32)
    normed = (
        inputs
        * lax.rsqrt(jnp.mean(inputs * inputs, axis=-1, keepdims=True) + norm_eps)
        * expert_gain
    ).astype(jnp.bfloat16)
    expert_ids = routes.reshape(-1)
    one_hot = (expert_ids[:, None] == jnp.arange(ep_count, dtype=jnp.int32)[None, :]).astype(
        jnp.int32
    )
    slot_index = jnp.sum((jnp.cumsum(one_hot, axis=0) - one_hot) * one_hot, axis=1)
    source_row = jnp.arange(row_count * pick_count, dtype=jnp.int32) // pick_count
    empty = jnp.zeros((ep_count, capacity, normed.shape[1]), jnp.bfloat16)
    arrived = lax.all_to_all(
        empty.at[expert_ids, slot_index].set(normed[source_row]),
        "ep",
        split_axis=0,
        concat_axis=0,
        tiled=True,
    )
    slot_count = arrived.shape[1]
    flat_rows = arrived.reshape(ep_count * slot_count, model_width)
    gate_values = jnp.dot(flat_rows, gate_weight[0], preferred_element_type=jnp.float32)
    up_values = jnp.dot(flat_rows, up_weight[0], preferred_element_type=jnp.float32)
    hidden = (jax.nn.silu(gate_values) * up_values).astype(jnp.bfloat16)
    partial_value = jnp.dot(hidden, down_weight[0], preferred_element_type=jnp.float32).reshape(
        ep_count, slot_count, model_width
    )
    summed = lax.psum_scatter(
        partial_value.astype(jnp.bfloat16), "tp", scatter_dimension=2, tiled=True
    )
    returned = lax.all_to_all(summed, "ep", split_axis=0, concat_axis=0, tiled=True)
    picked = returned[expert_ids, slot_index].reshape(row_count, pick_count, column_count)
    combined = jnp.sum(route_weights[..., None] * picked.astype(jnp.float32), axis=1)
    return combined.astype(jnp.bfloat16)


MESH = pl.DeviceIdType.MESH


def remote(source, target, send_sem, recv_sem, device):
    return pltpu.make_async_remote_copy(
        src_ref=source,
        dst_ref=target,
        send_sem=send_sem,
        recv_sem=recv_sem,
        device_id=device,
        device_id_type=MESH,
    )


def layer_kernel(
    n_ep,
    n_tp,
    rows_ref,
    norm_gain_ref,
    routes_ref,
    route_weights_ref,
    query_ref,
    key_ref,
    value_ref,
    cos_ref,
    sin_ref,
    lambda_ref,
    gain_ref,
    gate_hbm,
    up_hbm,
    down_hbm,
    weight_hbm,
    expert_ref,
    mixed_ref,
    slots_ref,
    all_ref,
    packed,
    gathered,
    gate_vmem,
    up_vmem,
    down_vmem,
    hidden,
    partial,
    arrived,
    summed,
    returned,
    weight_vmem,
    heads,
    landed,
    mixed_partial,
    mixed_arrived,
    weight_sem,
    local_sem,
    disp_send,
    disp_recv,
    gath_send,
    gath_recv,
    part_send,
    part_recv,
    ret_send,
    ret_recv,
    qkv_send,
    qkv_recv,
    pair_send,
    pair_recv,
    head_send,
    head_recv,
    mixed_send,
    mixed_recv,
):
    ep = lax.axis_index("ep")
    tp = lax.axis_index("tp")
    n_z = n_ep // 2
    z, core = ep // 2, lax.rem(ep, 2)
    capacity, width = slots_ref.shape[1:]
    rows = n_ep * capacity
    head_width = packed.shape[2] // 3
    half = head_width // 2
    weights = [
        pltpu.make_async_copy(gate_hbm, gate_vmem, weight_sem.at[0]),
        pltpu.make_async_copy(up_hbm, up_vmem, weight_sem.at[1]),
        pltpu.make_async_copy(down_hbm, down_vmem, weight_sem.at[2]),
        pltpu.make_async_copy(weight_hbm, weight_vmem, weight_sem.at[3]),
    ]
    for copy in weights:
        copy.start()
    peers = [{"ep": lax.rem(ep + d, n_ep)} for d in range(1, n_ep)]
    peers += [{"tp": lax.rem(tp + d, n_tp)} for d in range(1, n_tp)]
    barrier = pltpu.get_barrier_semaphore()
    for device in peers:
        pl.semaphore_signal(barrier, inc=1, device_id=device, device_id_type=MESH)

    token_count = rows_ref.shape[0]
    picks = routes_ref.shape[0]
    entries = rows_ref[...].astype(jnp.float32)
    inverse_norm = lax.rsqrt(jnp.mean(entries * entries, axis=1, keepdims=True) + norm_eps)
    own = pl.ds(pl.multiple_of(tp * width, width), width)
    normed = rows_ref[:, own].astype(jnp.float32) * inverse_norm * norm_gain_ref[:, own]
    normed = normed.astype(jnp.bfloat16)
    named_rows = -(-n_ep // 16) * 16
    label = lax.broadcasted_iota(jnp.int32, (named_rows, token_count), 0)
    named = [
        jnp.where(label == routes_ref[k : k + 1, :], 1.0, 0.0).astype(jnp.float32)
        for k in range(picks)
    ]
    before = lax.broadcasted_iota(jnp.int32, (token_count, token_count), 0)
    after = lax.broadcasted_iota(jnp.int32, (token_count, token_count), 1)
    earlier = jnp.dot(
        sum(named).astype(jnp.bfloat16),
        jnp.where(before < after, 1.0, 0.0).astype(jnp.bfloat16),
        preferred_element_type=jnp.float32,
    )
    slot_of = lax.broadcasted_iota(jnp.int32, (rows, token_count), 0)
    select = []
    for k in range(picks):
        rank = jnp.sum(named[k] * earlier, axis=0, keepdims=True).astype(jnp.int32)
        place = routes_ref[k : k + 1, :] * capacity + rank
        select.append(jnp.where(slot_of == place, 1.0, 0.0).astype(jnp.float32))
    slots_ref[...] = (
        jnp.dot(
            sum(select).astype(jnp.bfloat16), normed, preferred_element_type=jnp.float32
        )
        .astype(jnp.bfloat16)
        .reshape(n_ep, capacity, width)
    )
    pl.semaphore_wait(barrier, len(peers))
    mine = tp * n_ep + ep
    dispatch = [pltpu.make_async_copy(slots_ref.at[ep], gathered.at[mine], local_sem.at[0])]
    for d in range(1, n_ep):
        target = lax.rem(ep + d, n_ep)
        dispatch.append(
            remote(
                slots_ref.at[target],
                gathered.at[mine],
                disp_send.at[d],
                disp_recv.at[d],
                {"ep": target},
            )
        )
    for copy in dispatch:
        copy.start()

    for head in range(n_z):
        for index, ref in ((0, query_ref), (1, key_ref)):
            for m in range(2):
                at = head * head_width + m * half
                entry = ref[:, at : at + half].astype(jnp.float32)
                turned = entry * cos_ref[...] + pltpu.roll(entry, half // 2, 1) * sin_ref[...]
                to = index * head_width + m * half
                packed[head, :, to : to + half] = turned.astype(jnp.bfloat16)
        packed[head, :, 2 * head_width :] = value_ref[
            :, head * head_width : (head + 1) * head_width
        ]
    exchange = [pltpu.make_async_copy(packed.at[z], all_ref.at[ep], local_sem.at[1])]
    for d in range(1, n_z):
        target = lax.rem(z + d, n_z)
        exchange.append(
            remote(
                packed.at[target],
                all_ref.at[ep],
                qkv_send.at[d],
                qkv_recv.at[d],
                {"ep": 2 * target + core},
            )
        )
    for copy in exchange:
        copy.start()

    spread = []
    for d in range(n_ep):
        source = lax.rem(ep + n_ep - d, n_ep)
        if d == 0:
            dispatch[0].wait()
        else:
            dispatch[d].wait_recv()
        slot = gathered.at[tp * n_ep + source]
        for t in range(1, n_tp):
            copy = remote(
                slot,
                slot,
                gath_send.at[d * n_tp + t],
                gath_recv.at[d * n_tp + t],
                {"tp": lax.rem(tp + t, n_tp)},
            )
            copy.start()
            spread.append(copy)
    for copy in spread:
        copy.wait_recv()
    weights[0].wait()
    weights[1].wait()
    tile = 256

    def hidden_tile(j, carry):
        columns = pl.ds(pl.multiple_of(j * tile, tile), tile)
        gate = jnp.zeros((rows, tile), jnp.float32)
        up = jnp.zeros((rows, tile), jnp.float32)
        for i in range(n_tp):
            block = gathered[i * n_ep : (i + 1) * n_ep].reshape(rows, width)
            gate += jnp.dot(
                block,
                gate_vmem[0, i * width : (i + 1) * width, columns],
                preferred_element_type=jnp.float32,
            )
            up += jnp.dot(
                block,
                up_vmem[0, i * width : (i + 1) * width, columns],
                preferred_element_type=jnp.float32,
            )
        hidden[:, columns] = (gate / (1.0 + jnp.exp(-gate)) * up).astype(jnp.bfloat16)
        return carry

    lax.fori_loop(0, hidden.shape[1] // tile, hidden_tile, 0)
    weights[2].wait()
    scatter = []
    for d in list(range(1, n_tp)) + [0]:
        target = lax.rem(tp + d, n_tp)
        columns = pl.ds(pl.multiple_of(target * width, width), width)
        partial[d] = jnp.dot(
            hidden[...], down_vmem[0, :, columns], preferred_element_type=jnp.float32
        ).astype(jnp.bfloat16)
        if d:
            copy = remote(
                partial.at[d], arrived.at[d], part_send.at[d], part_recv.at[d], {"tp": target}
            )
            copy.start()
            scatter.append(copy)
    pairs = []
    for d in range(n_z):
        source = 2 * lax.rem(z + n_z - d, n_z) + core
        if d == 0:
            exchange[0].wait()
        else:
            exchange[d].wait_recv()
        part = all_ref.at[source, :, pl.ds(head_width, 2 * head_width)]
        copy = remote(part, part, pair_send.at[d], pair_recv.at[d], {"ep": ep + 1 - 2 * core})
        copy.start()
        pairs.append(copy)
    for copy in pairs:
        copy.wait_recv()

    row_count = all_ref.shape[1]
    value_width = head_width
    head_weight = jnp.sum(
        jnp.where(lax.broadcasted_iota(jnp.int32, lambda_ref.shape, 1) == z, lambda_ref[...], 0.0),
        axis=1,
        keepdims=True,
    )
    scale = half ** (-0.5)
    pair_rows = 2 * row_count
    row = lax.broadcasted_iota(jnp.int32, (row_count, pair_rows), 0) + core * row_count
    causal = lax.broadcasted_iota(jnp.int32, (row_count, pair_rows), 1) <= row

    def sender(block):
        return remote(
            heads.at[block],
            landed.at[z],
            head_send.at[block],
            head_recv.at[z],
            {"ep": 2 * block + core},
        )

    def keeper(block):
        return pltpu.make_async_copy(heads.at[block], landed.at[block], head_recv.at[block])

    def attend(block):
        maps = []
        for m in range(2):
            query = all_ref[2 * block + core, :, m * half : (m + 1) * half]
            pieces = []
            for pair in range(block + 1):
                at = value_width + m * half
                keys = all_ref[2 * pair : 2 * pair + 2, :, at : at + half].reshape(pair_rows, half)
                scores = lax.dot_general(
                    query, keys, (((1,), (1,)), ((), ())), preferred_element_type=jnp.float32
                )
                scores = scores * scale
                if pair == block:
                    scores = jnp.where(causal, scores, -1e30)
                pieces.append(scores)
            peak = functools.reduce(
                jnp.maximum, [jnp.max(piece, axis=1, keepdims=True) for piece in pieces]
            )
            total = jnp.zeros((row_count, 1), jnp.float32)
            outcome = jnp.zeros((row_count, value_width), jnp.float32)
            for pair in range(block + 1):
                expd = jnp.exp(pieces[pair] - peak)
                total += jnp.sum(expd, axis=1, keepdims=True)
                values = all_ref[2 * pair : 2 * pair + 2, :, 2 * value_width :].reshape(
                    pair_rows, value_width
                )
                outcome += jnp.dot(
                    expd.astype(jnp.bfloat16), values, preferred_element_type=jnp.float32
                )
            maps.append(outcome / total)
        difference = maps[0] - head_weight * maps[1]
        mean = jnp.mean(difference * difference, axis=1, keepdims=True)
        heads[block] = (difference * lax.rsqrt(mean + norm_eps) * gain_ref[...]).astype(
            jnp.bfloat16
        )

        @pl.when(z == block)
        def _():
            keeper(block).start()

        @pl.when(z != block)
        def _():
            sender(block).start()

    order = [n_z - 1] + [0] * (n_z > 1) + list(range(n_z - 2, 0, -1))
    for block in order[:2]:
        attend(block)
    total = partial[0].astype(jnp.float32)
    for d in range(1, n_tp):
        scatter[d - 1].wait_recv()
        total += arrived[d].astype(jnp.float32)
    summed[...] = total.astype(jnp.bfloat16).reshape(n_ep, capacity, width)
    back = [pltpu.make_async_copy(summed.at[ep], returned.at[ep], local_sem.at[2])]
    for d in range(1, n_ep):
        target = lax.rem(ep + d, n_ep)
        back.append(
            remote(
                summed.at[target],
                returned.at[ep],
                ret_send.at[d],
                ret_recv.at[d],
                {"ep": target},
            )
        )
    for copy in back:
        copy.start()

    for block in order[2:]:
        attend(block)
    back[0].wait()
    for copy in back[1:]:
        copy.wait_recv()
    flat = returned[...].reshape(rows, width)
    result = jnp.zeros(expert_ref.shape, jnp.float32)
    for k in range(picks):
        picked = lax.dot_general(
            select[k].astype(jnp.bfloat16),
            flat,
            (((0,), (0,)), ((), ())),
            preferred_element_type=jnp.float32,
        )
        spread_out = jnp.where(before == after, route_weights_ref[k : k + 1, :], 0.0)
        result += jnp.sum(spread_out, axis=1, keepdims=True) * picked
    expert_ref[...] = result.astype(expert_ref.dtype)
    for block in range(n_z):
        keeper(block).wait()
    weights[3].wait()
    mixed_scatter = []
    for d in list(range(1, n_tp)) + [0]:
        target = lax.rem(tp + d, n_tp)
        columns = pl.ds(pl.multiple_of(target * width, width), width)
        product = jnp.zeros((row_count, width), jnp.float32)
        for h in range(n_z):
            product += jnp.dot(
                landed[h],
                weight_vmem[h * value_width : (h + 1) * value_width, columns],
                preferred_element_type=jnp.float32,
            )
        mixed_partial[d] = product.astype(jnp.bfloat16)
        if d:
            copy = remote(
                mixed_partial.at[d], mixed_arrived.at[d], mixed_send.at[d], mixed_recv.at[d], {"tp": target}
            )
            copy.start()
            mixed_scatter.append(copy)
    total = mixed_partial[0].astype(jnp.float32)
    for d in range(1, n_tp):
        mixed_scatter[d - 1].wait_recv()
        total += mixed_arrived[d].astype(jnp.float32)
    mixed_ref[...] = total.astype(jnp.bfloat16)
    for copy in mixed_scatter:
        copy.wait_send()
    for block in range(n_z):

        @pl.when(z != block)
        def _():
            sender(block).wait_send()
    for copy in dispatch[1:] + exchange[1:] + spread + scatter + back[1:] + pairs:
        copy.wait_send()


def fused(
    query_maps,
    key_maps,
    value_rows,
    head_lambda,
    head_gain,
    out_weight,
    expert_rows,
    expert_gain,
    routes,
    route_weights,
    gate_weight,
    up_weight,
    down_weight,
):
    n_ep = lax.axis_size("ep")
    n_tp = lax.axis_size("tp")
    n_z = n_ep // 2
    ep = lax.axis_index("ep")
    row_count = query_maps.shape[0]
    head_width = query_maps.shape[1] // n_z
    head_dim = head_width // 2
    token_count, model_width = expert_rows.shape
    capacity = 3 * token_count * routes.shape[1] // (2 * n_ep)
    width = model_width // n_tp
    hidden_width = gate_weight.shape[2]
    slot_rows = n_ep * capacity

    positions = ep * row_count + jnp.arange(row_count, dtype=jnp.int32)
    half_dim = head_dim // 2
    inverse = rope_base ** (-2.0 * jnp.arange(half_dim, dtype=jnp.float32) / head_dim)
    angles = positions.astype(jnp.float32)[:, None] * inverse[None, :]
    cosine, sine = jnp.cos(angles), jnp.sin(angles)
    cos_table = jnp.concatenate([cosine, cosine], axis=1)
    sin_table = jnp.concatenate([-sine, sine], axis=1)

    vmem = pl.BlockSpec(memory_space=pltpu.VMEM)
    hbm = pl.BlockSpec(memory_space=pl.ANY)
    dma = pltpu.SemaphoreType.DMA
    bf16 = jnp.bfloat16
    expert_out, mixed = pl.pallas_call(
        functools.partial(layer_kernel, n_ep, n_tp),
        out_shape=(
            jax.ShapeDtypeStruct((token_count, width), bf16),
            jax.ShapeDtypeStruct((row_count, width), bf16),
        ),
        in_specs=[vmem] * 11 + [hbm] * 4,
        out_specs=(vmem, vmem),
        scratch_shapes=[
            pltpu.VMEM((n_ep, capacity, width), bf16),
            pltpu.VMEM((n_ep, row_count, 3 * head_width), bf16),
            pltpu.VMEM((n_z, row_count, 3 * head_width), bf16),
            pltpu.VMEM((n_tp * n_ep, capacity, width), bf16),
            pltpu.VMEM(gate_weight.shape, bf16),
            pltpu.VMEM(up_weight.shape, bf16),
            pltpu.VMEM(down_weight.shape, bf16),
            pltpu.VMEM((slot_rows, hidden_width), bf16),
            pltpu.VMEM((n_tp, slot_rows, width), bf16),
            pltpu.VMEM((n_tp, slot_rows, width), bf16),
            pltpu.VMEM((n_ep, capacity, width), bf16),
            pltpu.VMEM((n_ep, capacity, width), bf16),
            pltpu.VMEM(out_weight.shape, bf16),
            pltpu.VMEM((n_z, row_count, head_width), bf16),
            pltpu.VMEM((n_z, row_count, head_width), bf16),
            pltpu.VMEM((n_tp, row_count, width), bf16),
            pltpu.VMEM((n_tp, row_count, width), bf16),
            dma((4,)),
            dma((3,)),
            dma((n_ep,)),
            dma((n_ep,)),
            dma((n_ep * n_tp,)),
            dma((n_ep * n_tp,)),
            dma((n_tp,)),
            dma((n_tp,)),
            dma((n_ep,)),
            dma((n_ep,)),
            dma((n_z,)),
            dma((n_z,)),
            dma((n_z,)),
            dma((n_z,)),
            dma((n_z,)),
            dma((n_z,)),
            dma((n_tp,)),
            dma((n_tp,)),
        ],
        compiler_params=pltpu.CompilerParams(
            collective_id=0, has_side_effects=True, vmem_limit_bytes=60 * 1024 * 1024
        ),
        name="layer",
    )(
        expert_rows,
        expert_gain.reshape(1, model_width),
        routes.T,
        route_weights.T,
        query_maps,
        key_maps,
        value_rows,
        cos_table,
        sin_table,
        head_lambda.reshape(1, n_z),
        head_gain.reshape(1, head_width),
        gate_weight,
        up_weight,
        down_weight,
        out_weight,
    )
    return (mixed, expert_out)


def on_device(
    query_maps,
    key_maps,
    value_rows,
    head_lambda,
    head_gain,
    out_weight,
    expert_rows,
    expert_gain,
    routes,
    route_weights,
    gate_weight,
    up_weight,
    down_weight,
):
    n_ep = lax.axis_size("ep")
    head_count = head_lambda.shape[0]
    capacity = 3 * expert_rows.shape[0] * routes.shape[1] // (2 * n_ep)
    if (
        2 * head_count == n_ep
        and capacity % 16 == 0
        and value_rows.shape[1] == query_maps.shape[1] == 256 * head_count
    ):
        return fused(
            query_maps,
            key_maps,
            value_rows,
            head_lambda,
            head_gain,
            out_weight,
            expert_rows,
            expert_gain,
            routes,
            route_weights,
            gate_weight,
            up_weight,
            down_weight,
        )
    mixed = mixer_half(query_maps, key_maps, value_rows, head_lambda, head_gain, out_weight)
    expert_out = expert_half(
        expert_rows, expert_gain, routes, route_weights, gate_weight, up_weight, down_weight
    )
    return (mixed, expert_out)


def solution(mesh):
    placed = (
        P("ep", "tp"),
        P("ep", "tp"),
        P("ep", "tp"),
        P("tp"),
        P(),
        P("tp", None),
        P("ep", None),
        P(),
        P("ep", None),
        P("ep", None),
        P("ep", None, "tp"),
        P("ep", None, "tp"),
        P("ep", "tp", None),
    )
    return jax.shard_map(
        on_device,
        mesh=mesh,
        in_specs=placed,
        out_specs=(P("ep", "tp"), P("ep", "tp")),
        check_vma=False,
    )
```
